32 devices in a mesh: fs: 16 (over z, y, core), tp: 2 (over x).
Axes of the slice: x: 2, y: 2, z: 4, core: 2. Of those that a mesh axis runs over, the one named last changes fastest.
Arguments:
- tokens: bfloat16 [6144, 2048], P('fs', 'tp'), may hold values from -60 to 60
- gain_mixer: float32 [2048], P('tp'), may hold values from 0.1 to 1.9
- w_in: bfloat16 [2048, 1024], P('fs', 'tp'), may hold values from -0.125 to 0.125
- pool_scale: float32 [1024], P('tp'), may hold values from 0.1 to 1.9
- w_pool_out: bfloat16 [2048, 1024], P('fs', 'tp'), may hold values from -0.25 to 0.25
- gain_mid: float32 [2048], P('tp'), may hold values from 0.1 to 1.9
- w_ff1: bfloat16 [2048, 8192], P('fs', 'tp'), may hold values from -0.125 to 0.125
- w_ff2: bfloat16 [2048, 8192], P('fs', 'tp'), may hold values from -0.09375 to 0.09375
- gain_out: float32 [2048], P('tp'), may hold values from 0.1 to 1.9
Outputs:
- layer_out: bfloat16 [6144, 2048], P('fs', 'tp')
The draws below stay inside these ranges and needn't reach their ends.
All inputs are finite; a program needn't handle non-finite values.
Results may differ from the reference program's by a relative error of at most 0.017.
Values may be sent and summed in bfloat16 or wider, within the bound.
A program may use at most 128 MiB of HBM per device.

```python
import math
import jax
import jax.numpy as jnp
from jax import lax

D = 2048
POOL_WIDTH = 1024
FF = 8192
SEQ_DEV = 384
TOKENS = 6144
N_FS = 16
N_TP = 2


def draw_tokens(key, part):
    key_values = jax.random.fold_in(key, 11)
    key_rough = jax.random.fold_in(key, 12)
    column = jnp.arange(D, dtype=jnp.float32) / D
    rough = jax.random.uniform(key_rough, (D,), jnp.float32, 0.6, 1.5)
    scale = jnp.exp(math.log(4.0) * column) * rough
    values = jnp.clip(jax.random.normal(key_values, (TOKENS, D), jnp.float32), -6.0, 6.0)
    return (values * scale).astype(jnp.bfloat16)


def spiked(values, own_key, source, target, shards_of, factor):
    def block_of(dim):
        return (jnp.arange(values.shape[dim]) // (values.shape[dim] // shards_of)).reshape((-1,) + (1,) * (values.ndim - 1 - dim))

    first = jax.random.permutation(own_key, shards_of)[block_of(target)]
    second = (block_of(target) + shards_of // 2) % shards_of
    return jnp.where((block_of(source) == first) | (block_of(source) == second), factor * values, values)


def block_scale(key, dims, shards, low, top_value):
    factor_of, own = 1.0, jax.random.fold_in(key, 6)
    for dim, blocks in shards:
        heights = jnp.exp(jax.random.uniform(jax.random.fold_in(own, dim), (blocks,), jnp.float32, low / len(shards), top_value / len(shards)))
        factor_of = factor_of * jnp.repeat(heights, dims[dim] // blocks).reshape([-1 if axis == dim else 1 for axis in range(len(dims))])
    return factor_of


def noise(key, extent, scale, reach, split=(), kind=jnp.bfloat16):
    level = block_scale(key, extent, split, -0.22, 0.18) if split else 1.0
    drawn = jax.random.normal(key, extent, jnp.float32) * scale * level
    return jnp.minimum(jnp.maximum(drawn, -reach), reach).astype(kind)


def noise_with(key, shape, scale, bound, cuts, heavy, held_as=jnp.bfloat16):
    entries = scale * jax.random.normal(key, shape, jnp.float32)
    if cuts:
        entries = entries * block_scale(key, shape, cuts, -0.22, 0.18)
    return jnp.clip(spiked(entries, jax.random.fold_in(key, 3), *heavy), -bound, bound).astype(held_as)


def setup_inputs(seed: int = 0) -> dict:
    splits = jax.random.split(jax.random.key(seed), 10)
    return {
        "tokens": draw_tokens(jax.random.fold_in(splits[9], 71), 0),
        "gain_mixer": jnp.clip(1.0 + 0.18 * jax.random.normal(splits[1], (D,), jnp.float32), 0.1, 1.9),
        "w_in": noise(splits[2], (D, POOL_WIDTH), D ** -0.5, 0.125, ((0, 16), (1, 2))),
        "pool_scale": jnp.clip(1.0 + 0.18 * jax.random.normal(splits[3], (POOL_WIDTH,), jnp.float32), 0.1, 1.9),
        "w_pool_out": noise_with(splits[4], (D, POOL_WIDTH), POOL_WIDTH ** -0.5, 0.25, ((0, 16), (1, 2)), (1, 0, 16, 2.0)),
        "gain_mid": jnp.clip(1.0 + 0.18 * jax.random.normal(splits[5], (D,), jnp.float32), 0.1, 1.9),
        "w_ff1": noise(splits[6], (D, FF), D ** -0.5, 0.125, ((0, 16), (1, 2))),
        "w_ff2": noise_with(splits[7], (D, FF), FF ** -0.5, 0.09375, ((0, 16), (1, 2)), (1, 0, 16, 2.0)),
        "gain_out": jnp.clip(1.0 + 0.18 * jax.random.normal(splits[8], (D,), jnp.float32), 0.1, 1.9),
    }


norm_eps = 1e-05
residual_alpha = 2.0 ** 0.25

def norm_rows(value, gain):
    center = value - lax.optimization_barrier(jnp.mean(value, axis=-1, keepdims=True))
    spread = lax.optimization_barrier(jnp.mean(center * center, axis=-1, keepdims=True))
    return center * lax.rsqrt(spread + norm_eps) * gain

def block_sums(left, weight, blocks):
    width = left.shape[1] // blocks
    total = jnp.zeros((left.shape[0], weight.shape[0]), jnp.float32)
    for block in range(blocks):
        term = lax.dot_general(left[:, block * width:(block + 1) * width], weight[:, block * width:(block + 1) * width], (((1,), (1,)), ((), ())), preferred_element_type=jnp.float32)
        term = lax.optimization_barrier(term.astype(jnp.bfloat16))
        total = total + term.astype(jnp.float32)
    return total.astype(jnp.bfloat16)

def reference(tokens, gain_mixer, w_in, pool_scale, w_pool_out, gain_mid, w_ff1, w_ff2, gain_out):
    group = POOL_WIDTH // 4

    def one_sequence(seq_rows):
        xf = seq_rows.astype(jnp.float32)
        mixed_in = norm_rows(xf, gain_mixer).astype(jnp.bfloat16)
        pool_in = jnp.dot(mixed_in, w_in, preferred_element_type=jnp.float32).astype(jnp.bfloat16)
        uf = pool_in.astype(jnp.float32)
        length = uf.shape[0]
        sums = jnp.pad(jnp.cumsum(uf, axis=0), ((1, 0), (0, 0)))
        position = jnp.arange(length, dtype=jnp.float32)[:, None]
        pieces = []
        for index, window in enumerate((2, 4, 8, 16)):
            part = sums[:, index * group:(index + 1) * group]
            upper = part[1:]
            lower = jnp.pad(part, ((window - 1, 0), (0, 0)))[:length]
            count = jnp.minimum(position + 1.0, float(window))
            pieces.append((upper - lower) / count - uf[:, index * group:(index + 1) * group])
        pooled = (jnp.concatenate(pieces, axis=1) * pool_scale).astype(jnp.bfloat16)
        mixer_out = block_sums(pooled, w_pool_out, N_TP)
        middle = norm_rows(residual_alpha * xf + mixer_out.astype(jnp.float32), gain_mid).astype(jnp.bfloat16)
        upward = jnp.dot(middle, w_ff1, preferred_element_type=jnp.float32)
        hidden = jnp.square(jax.nn.relu(upward)).astype(jnp.bfloat16)
        ff_out = block_sums(hidden, w_ff2, N_TP)
        result = norm_rows(residual_alpha * middle.astype(jnp.float32) + ff_out.astype(jnp.float32), gain_out)
        return result.astype(jnp.bfloat16)
    stacked = tokens.reshape(N_FS, SEQ_DEV, D)
    return lax.map(one_sequence, stacked).reshape(N_FS * SEQ_DEV, D)
```

```python
import functools
import math

import jax
import jax.numpy as jnp
from jax import lax
from jax.experimental import pallas as pl
from jax.experimental.pallas import tpu as pltpu
from jax.sharding import PartitionSpec as P

norm_eps = 1e-05
residual_alpha = 2.0**0.25
f32, bf16 = jnp.float32, jnp.bfloat16
MESH = pl.DeviceIdType.MESH


def nt_dot(left, right):
    return lax.dot_general(left, right, (((1,), (1,)), ((), ())), preferred_element_type=f32)


def kernel(
    n, tps,
    x_ref, gains_ref, scale_ref, gout_ref, win_ref, wpo_ref, wup_ref, wdn_ref, out_ref,
    win, wpo, wup, wdn, xfull, gfull, mixed, mpart, mrecv, middle, hidden, part, precv, work,
    load_sem, is_sem, ir_sem, ds_sem, dr_sem, xs_sem, xr_sem, gs_sem, gr_sem,
    ms_sem, mr_sem, ps_sem, pr_sem,
):
    i, t = lax.axis_index("fs"), lax.axis_index("tp")
    core, chip = lax.rem(i, 2), lax.div(i, 2)
    half = n // 2
    rows, feat = x_ref.shape
    cin = win_ref.shape[1]
    width = feat * tps
    own = win_ref.shape[0]
    rh = own // 2
    rc = own * 2
    ffw = wup_ref.shape[1]
    fh = ffw // 2

    pos = jnp.where(lax.rem(chip, 2) == 0, lax.div(chip, 2), n - 1 - lax.div(chip, 2))

    def chip_at(p):
        q = lax.rem(p + 2 * n, n)
        return jnp.where(q < half, 2 * q, 2 * (n - 1 - q) + 1)

    sib = chip * 2 + (1 - core)
    ring = [chip_at(pos + 1) * 2 + core, chip_at(pos - 1) * 2 + core]
    peers = [lax.rem(t + q, tps) for q in range(1, tps)]

    streams = [(win, 0, cin), (wpo, 0, cin), (wup, 0, fh), (wup, fh, fh), (wdn, 0, fh), (wdn, fh, fh)]

    def block(w, where, c, d):
        ref, c0, cw = streams[w]
        r0 = pl.multiple_of((where * 2 + c) * own + d * rh, rh)
        return ref.at[pl.ds(r0, rh), pl.ds(c0, cw)]

    def source(s, d):
        return chip_at(pos - s) if d == 0 else chip_at(pos + s)

    def hop(w, s, d):
        b = block(w, source(s, d), core, d)
        return pltpu.make_async_remote_copy(
            b, b, is_sem.at[w, s, d], ir_sem.at[w, s, d], device_id=(ring[d], t), device_id_type=MESH)

    def share(w, s, d):
        b = block(w, source(s, d), core, d)
        return pltpu.make_async_remote_copy(
            b, b, ds_sem.at[w, s, d], dr_sem.at[w, s, d], device_id=(sib, t), device_id_type=MESH)

    def begin(w):
        for d in range(2):
            hop(w, 0, d).start()
        for d in range(2):
            share(w, 0, d).start()

    def advance(ws, s, last=False):
        for w in ws:
            for d in range(2):
                hop(w, s, d).wait_recv()
                if not last:
                    hop(w, s + 1, d).start()
                share(w, s + 1, d).start()

    def run(ws, lo, hi):
        def body(s, carry):
            advance(ws, s)
            return carry
        lax.fori_loop(lo, hi, body, 0)

    def shared(w):
        def body(s, carry):
            for d in range(2):
                share(w, s, d).wait_recv()
            return carry
        lax.fori_loop(0, n, body, 0)

    barrier = pltpu.get_barrier_semaphore()
    for f in ring + [sib]:
        pl.semaphore_signal(barrier, inc=1, device_id=(f, t), device_id_type=MESH)
    for p in peers:
        pl.semaphore_signal(barrier, inc=1, device_id=(i, p), device_id_type=MESH)
    loads = []
    mine = pl.ds(pl.multiple_of(i * own, own), own)
    for k, (src, dst) in enumerate(((win_ref, win), (wpo_ref, wpo), (wup_ref, wup), (wdn_ref, wdn))):
        loads.append(pltpu.make_async_copy(src, dst.at[mine], load_sem.at[k]))
        loads[-1].start()
    pl.semaphore_wait(barrier, 3 + len(peers))

    def x_copy(q):
        return pltpu.make_async_remote_copy(
            x_ref, xfull.at[t], xs_sem.at[q], xr_sem.at[q], device_id=(i, peers[q]), device_id_type=MESH)

    def g_copy(q):
        return pltpu.make_async_remote_copy(
            gains_ref, gfull.at[t], gs_sem.at[q], gr_sem.at[q], device_id=(i, peers[q]), device_id_type=MESH)

    for w in range(2):
        loads[w].wait()
        begin(w)
    for q in range(tps - 1):
        x_copy(q).start()
        g_copy(q).start()
    xfull[t] = x_ref[...]
    gfull[t] = gains_ref[...]

    run((0, 1), 0, n - 2)
    loads[2].wait()
    begin(2)
    begin(3)
    advance((0, 1), n - 2, last=True)
    loads[3].wait()

    rb = math.gcd(rows, 32)

    def blocks_of(body):
        def step(r, carry):
            body(pl.ds(pl.multiple_of(r * rb, rb), rb))
            return carry
        lax.fori_loop(0, rows // rb, step, 0)

    def norm(pieces):
        total = sum(jnp.sum(v, axis=1, keepdims=True) for v in pieces)
        mean = total / width
        pieces = [v - mean for v in pieces]
        spread = sum(jnp.sum(v * v, axis=1, keepdims=True) for v in pieces) / width
        inv = lax.rsqrt(spread + norm_eps)
        return [v * inv for v in pieces]

    for q in range(tps - 1):
        x_copy(q).wait_recv()
        g_copy(q).wait_recv()

    def first_norm(rs):
        pieces = norm([xfull[r, rs, :].astype(f32) for r in range(tps)])
        for r in range(tps):
            mixed[rs, r * feat:(r + 1) * feat] = (pieces[r] * gfull[r, 0:1, :]).astype(bf16)

    blocks_of(first_norm)
    shared(0)
    cb = math.gcd(cin, 128)
    gw = cin * tps // 4
    pool = jnp.dot(mixed[...], win[...], preferred_element_type=f32)
    work[:, :cin] = pool.astype(bf16).astype(f32)
    row = lax.broadcasted_iota(jnp.int32, (rows, cb), 0)
    position = (row + 1).astype(f32)
    pooled = []
    for c in range(cin // cb):
        cs = slice(c * cb, (c + 1) * cb)
        u = work[:, cs]

        def shifted(v, steps):
            return jnp.where(row >= steps, pltpu.roll(v, steps, axis=0), 0.0)

        s2 = u + shifted(u, 1)
        s4 = s2 + shifted(s2, 2)
        s8 = s4 + shifted(s4, 4)
        s16 = s8 + shifted(s8, 8)
        channel = t * cin + c * cb + lax.broadcasted_iota(jnp.int32, (rows, cb), 1)

        def pick(a, b, e, g):
            return jnp.where(channel < gw, a, jnp.where(channel < 2 * gw, b, jnp.where(channel < 3 * gw, e, g)))

        count = jnp.minimum(position, pick(2.0, 4.0, 8.0, 16.0))
        mixed[:, cs] = ((pick(s2, s4, s8, s16) / count - u) * scale_ref[0:1, cs]).astype(bf16)

    def m_copy(q):
        return pltpu.make_async_remote_copy(
            mpart, mrecv.at[q], ms_sem.at[q], mr_sem.at[q], device_id=(i, peers[q]), device_id_type=MESH)

    shared(1)
    wb = math.gcd(width, 512)

    def out_proj(k, carry):
        cs = pl.ds(pl.multiple_of(k * wb, wb), wb)
        mpart[:, cs] = nt_dot(mixed[:, :cin], wpo[cs, :]).astype(bf16)
        return carry

    lax.fori_loop(0, width // wb, out_proj, 0)
    for q in range(tps - 1):
        m_copy(q).start()

    run((2, 3), 0, half)
    for q in range(tps - 1):
        m_copy(q).wait_recv()

    def second_norm(rs):
        pieces = []
        for r in range(tps):
            cs = slice(r * feat, (r + 1) * feat)
            mix = mpart[rs, cs].astype(f32)
            for q in range(tps - 1):
                mix = mix + mrecv[q, rs, cs].astype(f32)
            mix = mix.astype(bf16).astype(f32)
            pieces.append(residual_alpha * xfull[r, rs, :].astype(f32) + mix)
        pieces = norm(pieces)
        for r in range(tps):
            middle[rs, r * feat:(r + 1) * feat] = (pieces[r] * gfull[r, 1:2, :]).astype(bf16)

    blocks_of(second_norm)
    run((2, 3), half, n - 2)
    begin(4)
    begin(5)
    advance((2, 3), n - 2, last=True)
    shared(2)
    shared(3)

    hb = math.gcd(ffw, 512)
    chunks = ffw // hb

    def up(k, carry):
        cs = pl.ds(pl.multiple_of(k * hb, hb), hb)
        act = jnp.maximum(jnp.dot(middle[...], wup[:, cs], preferred_element_type=f32), 0.0)
        hidden[:, cs] = (act * act).astype(bf16)
        return carry

    third = -(-chunks // 3)
    lax.fori_loop(0, third, up, 0)
    advance((4,), 0)
    lax.fori_loop(third, min(2 * third, chunks), up, 0)
    advance((5,), 0)
    lax.fori_loop(min(2 * third, chunks), chunks, up, 0)

    def p_copy(q, k):
        return pltpu.make_async_remote_copy(
            part.at[k], precv.at[q, k], ps_sem.at[q, k], pr_sem.at[q, k],
            device_id=(i, peers[q]), device_id_type=MESH)

    def down(distance):
        for w in (4, 5):
            share(w, distance, 0).wait_recv()
            share(w, lax.rem(n - distance, n), 1).wait_recv()
        k = chip_at(pos - distance)
        part[k] = nt_dot(hidden[...], wdn[pl.ds(pl.multiple_of(k * rc, rc), rc), :]).astype(bf16)
        for q in range(tps - 1):
            p_copy(q, k).start()

    advance((4, 5), 1)
    run((4, 5), 2, half - 1)

    def first_two(j, carry):
        down(j * half)
        return carry

    def last_two(s):
        def body(j, carry):
            down(jnp.where(j == 0, s + 1, n - 1 - s))
            return carry
        lax.fori_loop(0, 2, body, 0)

    advance((4, 5), half - 1)
    lax.fori_loop(0, 2, first_two, 0)

    def tail(s, carry):
        advance((4, 5), s)
        last_two(s)
        return carry

    lax.fori_loop(half, n - 2, tail, 0)
    advance((4, 5), n - 2, last=True)
    last_two(n - 2)

    for q in range(tps - 1):
        def arrived(k, carry):
            p_copy(q, k).wait_recv()
            return carry
        lax.fori_loop(0, n, arrived, 0)

    per = n // tps

    def last_norm(rs):
        total = jnp.zeros((rb, 1), f32)
        values = []
        for k in range(n):
            ff = part[k, rs, :].astype(f32)
            for q in range(tps - 1):
                ff = ff + precv[q, k, rs, :].astype(f32)
            v = residual_alpha * middle[rs, k * rc:(k + 1) * rc].astype(f32) + ff.astype(bf16).astype(f32)
            values.append(v)
            total = total + jnp.sum(v, axis=1, keepdims=True)
        mean = total / width
        square = jnp.zeros((rb, 1), f32)
        for v in values:
            square = square + jnp.sum((v - mean) * (v - mean), axis=1, keepdims=True)
        inv = lax.rsqrt(square / width + norm_eps)
        for j in range(per):
            v = values[j]
            for r in range(1, tps):
                v = jnp.where(t == r, values[r * per + j], v)
            cs = slice(j * rc, (j + 1) * rc)
            out_ref[rs, cs] = ((v - mean) * inv * gout_ref[0:1, cs]).astype(bf16)

    blocks_of(last_norm)

    for q in range(tps - 1):
        x_copy(q).wait_send()
        g_copy(q).wait_send()
        m_copy(q).wait_send()

        def sent(k, carry):
            p_copy(q, k).wait_send()
            return carry
        lax.fori_loop(0, n, sent, 0)

    def drained(s, carry):
        for w in range(len(streams)):
            for d in range(2):
                hop(w, s, d).wait_send()
                share(w, s, d).wait_send()
        return carry

    lax.fori_loop(0, n - 1, drained, 0)
    for w in range(len(streams)):
        for d in range(2):
            share(w, n - 1, d).wait_send()


def local(n, tps, tokens, gain_mixer, w_in, pool_scale, w_pool_out, gain_mid, w_ff1, w_ff2, gain_out):
    rows, feat = tokens.shape
    own, cin = w_in.shape
    ffw = w_ff1.shape[1]
    width = feat * tps
    rc = own * 2
    gains = jnp.stack([gain_mixer, gain_mid])
    vmem, hbm = pl.BlockSpec(memory_space=pltpu.VMEM), pl.BlockSpec(memory_space=pl.ANY)
    dma = pltpu.SemaphoreType.DMA
    lanes = tps - 1
    return pl.pallas_call(
        functools.partial(kernel, n, tps),
        out_shape=jax.ShapeDtypeStruct((rows, feat), bf16),
        in_specs=[vmem] * 4 + [hbm] * 4,
        out_specs=vmem,
        scratch_shapes=[
            pltpu.VMEM((width, cin), bf16),
            pltpu.VMEM((width, cin), bf16),
            pltpu.VMEM((width, ffw), bf16),
            pltpu.VMEM((width, ffw), bf16),
            pltpu.VMEM((tps, rows, feat), bf16),
            pltpu.VMEM((tps, 2, feat), f32),
            pltpu.VMEM((rows, width), bf16),
            pltpu.VMEM((rows, width), bf16),
            pltpu.VMEM((lanes, rows, width), bf16),
            pltpu.VMEM((rows, width), bf16),
            pltpu.VMEM((rows, ffw), bf16),
            pltpu.VMEM((n, rows, rc), bf16),
            pltpu.VMEM((lanes, n, rows, rc), bf16),
            pltpu.VMEM((rows, cin), f32),
            dma((4,)),
            dma((6, n, 2)), dma((6, n, 2)), dma((6, n, 2)), dma((6, n, 2)),
            dma((lanes,)), dma((lanes,)), dma((lanes,)), dma((lanes,)),
            dma((lanes,)), dma((lanes,)), dma((lanes, n)), dma((lanes, n)),
        ],
        compiler_params=pltpu.CompilerParams(
            collective_id=0, has_side_effects=True, vmem_limit_bytes=67043328
        ),
    )(tokens, gains, pool_scale[None], gain_out[None], w_in, w_pool_out, w_ff1, w_ff2)


def solution(mesh):
    n, tps = mesh.shape["fs"] // 2, mesh.shape["tp"]
    return jax.shard_map(
        functools.partial(local, n, tps),
        mesh=mesh,
        in_specs=(
            P("fs", "tp"),
            P("tp"),
            P("fs", "tp"),
            P("tp"),
            P("fs", "tp"),
            P("tp"),
            P("fs", "tp"),
            P("fs", "tp"),
            P("tp"),
        ),
        out_specs=P("fs", "tp"),
        check_vma=False,
    )
```

```python
import functools
import math

import jax
import jax.numpy as jnp
from jax import lax
from jax.experimental import pallas as pl
from jax.experimental.pallas import tpu as pltpu
from jax.sharding import PartitionSpec as P

norm_eps = 1e-05
residual_alpha = 2.0**0.25
f32, bf16 = jnp.float32, jnp.bfloat16
MESH = pl.DeviceIdType.MESH


def nt_dot(left, right):
    return lax.dot_general(left, right, (((1,), (1,)), ((), ())), preferred_element_type=f32)


def kernel(
    n, tps,
    x_ref, gains_ref, scale_ref, gout_ref, win_ref, wpo_ref, wup_ref, wdn_ref, out_ref,
    win, wpo, wup, wdn, xfull, gfull, mixed, mpart, mrecv, middle, hidden, part, precv, work,
    load_sem, is_sem, ir_sem, ds_sem, dr_sem, xs_sem, xr_sem, gs_sem, gr_sem,
    ms_sem, mr_sem, ps_sem, pr_sem,
):
    i, t = lax.axis_index("fs"), lax.axis_index("tp")
    core, chip = lax.rem(i, 2), lax.div(i, 2)
    half = n // 2
    rows, feat = x_ref.shape
    cin = win_ref.shape[1]
    width = feat * tps
    own = win_ref.shape[0]
    rh = own // 2
    rc = own * 2
    ffw = wup_ref.shape[1]
    fh = ffw // 2

    pos = jnp.where(lax.rem(chip, 2) == 0, lax.div(chip, 2), n - 1 - lax.div(chip, 2))

    def chip_at(p):
        q = lax.rem(p + 2 * n, n)
        return jnp.where(q < half, 2 * q, 2 * (n - 1 - q) + 1)

    sib = chip * 2 + (1 - core)
    ring = [chip_at(pos + 1) * 2 + core, chip_at(pos - 1) * 2 + core]
    peers = [lax.rem(t + q, tps) for q in range(1, tps)]

    streams = [(win, 0, cin), (wpo, 0, cin), (wup, 0, fh), (wup, fh, fh), (wdn, 0, fh), (wdn, fh, fh)]

    def block(w, where, c, d):
        ref, c0, cw = streams[w]
        r0 = pl.multiple_of((where * 2 + c) * own + d * rh, rh)
        return ref.at[pl.ds(r0, rh), pl.ds(c0, cw)]

    def source(s, d):
        return chip_at(pos - s) if d == 0 else chip_at(pos + s)

    def hop(w, s, d):
        b = block(w, source(s, d), core, d)
        return pltpu.make_async_remote_copy(
            b, b, is_sem.at[w, s, d], ir_sem.at[w, s, d], device_id=(ring[d], t), device_id_type=MESH)

    def share(w, s, d):
        b = block(w, source(s, d), core, d)
        return pltpu.make_async_remote_copy(
            b, b, ds_sem.at[w, s, d], dr_sem.at[w, s, d], device_id=(sib, t), device_id_type=MESH)

    def begin(w):
        for d in range(2):
            hop(w, 0, d).start()
        for d in range(2):
            share(w, 0, d).start()

    def advance(ws, s, last=False):
        for w in ws:
            for d in range(2):
                hop(w, s, d).wait_recv()
                if not last:
                    hop(w, s + 1, d).start()
                share(w, s + 1, d).start()

    def run(ws, lo, hi):
        def body(s, carry):
            advance(ws, s)
            return carry
        lax.fori_loop(lo, hi, body, 0)

    def shared(w):
        def body(s, carry):
            for d in range(2):
                share(w, s, d).wait_recv()
            return carry
        lax.fori_loop(0, n, body, 0)

    barrier = pltpu.get_barrier_semaphore()
    for f in ring + [sib]:
        pl.semaphore_signal(barrier, inc=1, device_id=(f, t), device_id_type=MESH)
    for p in peers:
        pl.semaphore_signal(barrier, inc=1, device_id=(i, p), device_id_type=MESH)
    loads = []
    mine = pl.ds(pl.multiple_of(i * own, own), own)
    for k, (src, dst) in enumerate(((win_ref, win), (wpo_ref, wpo), (wup_ref, wup), (wdn_ref, wdn))):
        loads.append(pltpu.make_async_copy(src, dst.at[mine], load_sem.at[k]))
        loads[-1].start()
    pl.semaphore_wait(barrier, 3 + len(peers))

    def x_copy(q):
        return pltpu.make_async_remote_copy(
            x_ref, xfull.at[t], xs_sem.at[q], xr_sem.at[q], device_id=(i, peers[q]), device_id_type=MESH)

    def g_copy(q):
        return pltpu.make_async_remote_copy(
            gains_ref, gfull.at[t], gs_sem.at[q], gr_sem.at[q], device_id=(i, peers[q]), device_id_type=MESH)

    for w in range(2):
        loads[w].wait()
        begin(w)
    for q in range(tps - 1):
        x_copy(q).start()
        g_copy(q).start()
    loads[2].wait()
    begin(2)
    xfull[t] = x_ref[...]
    gfull[t] = gains_ref[...]

    advance((0, 1), 0)
    begin(3)

    pairs = (n - 3) // 2

    def both(s, carry):
        advance((0, 1), 2 * s + 1)
        advance((2,), s)
        advance((0, 1), 2 * s + 2)
        advance((3,), s)
        return carry

    lax.fori_loop(0, pairs, both, 0)
    run((0, 1), 2 * pairs + 1, n - 2)
    advance((0, 1), n - 2, last=True)
    loads[3].wait()

    rb = math.gcd(rows, 32)

    def blocks_of(body):
        def step(r, carry):
            body(pl.ds(pl.multiple_of(r * rb, rb), rb))
            return carry
        lax.fori_loop(0, rows // rb, step, 0)

    def norm(pieces):
        total = sum(jnp.sum(v, axis=1, keepdims=True) for v in pieces)
        mean = total / width
        pieces = [v - mean for v in pieces]
        spread = sum(jnp.sum(v * v, axis=1, keepdims=True) for v in pieces) / width
        inv = lax.rsqrt(spread + norm_eps)
        return [v * inv for v in pieces]

    for q in range(tps - 1):
        x_copy(q).wait_recv()
        g_copy(q).wait_recv()

    def first_norm(rs):
        pieces = norm([xfull[r, rs, :].astype(f32) for r in range(tps)])
        for r in range(tps):
            mixed[rs, r * feat:(r + 1) * feat] = (pieces[r] * gfull[r, 0:1, :]).astype(bf16)

    blocks_of(first_norm)
    shared(0)
    cb = math.gcd(cin, 128)
    gw = cin * tps // 4
    pool = jnp.dot(mixed[...], win[...], preferred_element_type=f32)
    work[:, :cin] = pool.astype(bf16).astype(f32)
    row = lax.broadcasted_iota(jnp.int32, (rows, cb), 0)
    position = (row + 1).astype(f32)
    pooled = []
    for c in range(cin // cb):
        cs = slice(c * cb, (c + 1) * cb)
        u = work[:, cs]

        def shifted(v, steps):
            return jnp.where(row >= steps, pltpu.roll(v, steps, axis=0), 0.0)

        s2 = u + shifted(u, 1)
        s4 = s2 + shifted(s2, 2)
        s8 = s4 + shifted(s4, 4)
        s16 = s8 + shifted(s8, 8)
        channel = t * cin + c * cb + lax.broadcasted_iota(jnp.int32, (rows, cb), 1)

        def pick(a, b, e, g):
            return jnp.where(channel < gw, a, jnp.where(channel < 2 * gw, b, jnp.where(channel < 3 * gw, e, g)))

        count = jnp.minimum(position, pick(2.0, 4.0, 8.0, 16.0))
        mixed[:, cs] = ((pick(s2, s4, s8, s16) / count - u) * scale_ref[0:1, cs]).astype(bf16)

    def m_copy(q):
        return pltpu.make_async_remote_copy(
            mpart, mrecv.at[q], ms_sem.at[q], mr_sem.at[q], device_id=(i, peers[q]), device_id_type=MESH)

    shared(1)
    wb = math.gcd(width, 512)

    def out_proj(k, carry):
        cs = pl.ds(pl.multiple_of(k * wb, wb), wb)
        mpart[:, cs] = nt_dot(mixed[:, :cin], wpo[cs, :]).astype(bf16)
        return carry

    lax.fori_loop(0, width // wb, out_proj, 0)
    for q in range(tps - 1):
        m_copy(q).start()

    run((2, 3), pairs, min(half + 2, n - 2))
    for q in range(tps - 1):
        m_copy(q).wait_recv()

    def second_norm(rs):
        pieces = []
        for r in range(tps):
            cs = slice(r * feat, (r + 1) * feat)
            mix = mpart[rs, cs].astype(f32)
            for q in range(tps - 1):
                mix = mix + mrecv[q, rs, cs].astype(f32)
            mix = mix.astype(bf16).astype(f32)
            pieces.append(residual_alpha * xfull[r, rs, :].astype(f32) + mix)
        pieces = norm(pieces)
        for r in range(tps):
            middle[rs, r * feat:(r + 1) * feat] = (pieces[r] * gfull[r, 1:2, :]).astype(bf16)

    blocks_of(second_norm)
    run((2, 3), min(half + 2, n - 2), n - 2)
    begin(4)
    begin(5)
    advance((2, 3), n - 2, last=True)
    shared(2)
    shared(3)

    hb = math.gcd(ffw, 512)
    chunks = ffw // hb

    def up(k, carry):
        cs = pl.ds(pl.multiple_of(k * hb, hb), hb)
        act = jnp.maximum(jnp.dot(middle[...], wup[:, cs], preferred_element_type=f32), 0.0)
        hidden[:, cs] = (act * act).astype(bf16)
        return carry

    third = -(-chunks // 3)
    lax.fori_loop(0, third, up, 0)
    advance((4,), 0)
    lax.fori_loop(third, min(2 * third, chunks), up, 0)
    advance((5,), 0)
    lax.fori_loop(min(2 * third, chunks), chunks, up, 0)

    def p_copy(q, k):
        return pltpu.make_async_remote_copy(
            part.at[k], precv.at[q, k], ps_sem.at[q, k], pr_sem.at[q, k],
            device_id=(i, peers[q]), device_id_type=MESH)

    def down(s):
        for w in (4, 5):
            for d in range(2):
                share(w, s, d).wait_recv()
        pieces = []
        for d in range(2):
            for c in range(2):
                r0 = pl.multiple_of((source(s, d) * 2 + c) * own + d * rh, rh)
                pieces.append(wdn[pl.ds(r0, rh), :])
        part[s] = nt_dot(hidden[...], jnp.concatenate(pieces, axis=0)).astype(bf16)
        for q in range(tps - 1):
            p_copy(q, s).start()

    def tail(s, carry):
        advance((4, 5), s)
        down(s)
        return carry

    down(0)
    lax.fori_loop(1, n - 2, tail, 0)
    down(n - 2)
    advance((4, 5), n - 2, last=True)
    down(n - 1)

    for q in range(tps - 1):
        def arrived(k, carry):
            p_copy(q, k).wait_recv()
            return carry
        lax.fori_loop(0, n, arrived, 0)

    per = n // tps

    def last_norm(rs):
        total = jnp.zeros((rb, 1), f32)
        values = []
        for k in range(n):
            at = k // 2 if k % 2 == 0 else n - 1 - k // 2
            sides = []
            for d in range(2):
                s = lax.rem((pos - at if d == 0 else at - pos) + n, n)
                cs = slice(d * own, (d + 1) * own)
                ff = part[s, rs, cs].astype(f32)
                for q in range(tps - 1):
                    ff = ff + precv[q, s, rs, cs].astype(f32)
                sides.append(ff)
            ff = jnp.concatenate(
                [sides[d][:, c * rh:(c + 1) * rh] for c in range(2) for d in range(2)], axis=1)
            v = residual_alpha * middle[rs, k * rc:(k + 1) * rc].astype(f32) + ff.astype(bf16).astype(f32)
            values.append(v)
            total = total + jnp.sum(v, axis=1, keepdims=True)
        mean = total / width
        square = jnp.zeros((rb, 1), f32)
        for v in values:
            square = square + jnp.sum((v - mean) * (v - mean), axis=1, keepdims=True)
        inv = lax.rsqrt(square / width + norm_eps)
        for j in range(per):
            v = values[j]
            for r in range(1, tps):
                v = jnp.where(t == r, values[r * per + j], v)
            cs = slice(j * rc, (j + 1) * rc)
            out_ref[rs, cs] = ((v - mean) * inv * gout_ref[0:1, cs]).astype(bf16)

    blocks_of(last_norm)

    for q in range(tps - 1):
        x_copy(q).wait_send()
        g_copy(q).wait_send()
        m_copy(q).wait_send()

        def sent(k, carry):
            p_copy(q, k).wait_send()
            return carry
        lax.fori_loop(0, n, sent, 0)

    def drained(s, carry):
        for w in range(len(streams)):
            for d in range(2):
                hop(w, s, d).wait_send()
                share(w, s, d).wait_send()
        return carry

    lax.fori_loop(0, n - 1, drained, 0)
    for w in range(len(streams)):
        for d in range(2):
            share(w, n - 1, d).wait_send()


def local(n, tps, tokens, gain_mixer, w_in, pool_scale, w_pool_out, gain_mid, w_ff1, w_ff2, gain_out):
    rows, feat = tokens.shape
    own, cin = w_in.shape
    ffw = w_ff1.shape[1]
    width = feat * tps
    rc = own * 2
    gains = jnp.stack([gain_mixer, gain_mid])
    vmem, hbm = pl.BlockSpec(memory_space=pltpu.VMEM), pl.BlockSpec(memory_space=pl.ANY)
    dma = pltpu.SemaphoreType.DMA
    lanes = tps - 1
    return pl.pallas_call(
        functools.partial(kernel, n, tps),
        out_shape=jax.ShapeDtypeStruct((rows, feat), bf16),
        in_specs=[vmem] * 4 + [hbm] * 4,
        out_specs=vmem,
        scratch_shapes=[
            pltpu.VMEM((width, cin), bf16),
            pltpu.VMEM((width, cin), bf16),
            pltpu.VMEM((width, ffw), bf16),
            pltpu.VMEM((width, ffw), bf16),
            pltpu.VMEM((tps, rows, feat), bf16),
            pltpu.VMEM((tps, 2, feat), f32),
            pltpu.VMEM((rows, width), bf16),
            pltpu.VMEM((rows, width), bf16),
            pltpu.VMEM((lanes, rows, width), bf16),
            pltpu.VMEM((rows, width), bf16),
            pltpu.VMEM((rows, ffw), bf16),
            pltpu.VMEM((n, rows, rc), bf16),
            pltpu.VMEM((lanes, n, rows, rc), bf16),
            pltpu.VMEM((rows, cin), f32),
            dma((4,)),
            dma((6, n, 2)), dma((6, n, 2)), dma((6, n, 2)), dma((6, n, 2)),
            dma((lanes,)), dma((lanes,)), dma((lanes,)), dma((lanes,)),
            dma((lanes,)), dma((lanes,)), dma((lanes, n)), dma((lanes, n)),
        ],
        compiler_params=pltpu.CompilerParams(
            collective_id=0, has_side_effects=True, vmem_limit_bytes=67043328
        ),
    )(tokens, gains, pool_scale[None], gain_out[None], w_in, w_pool_out, w_ff1, w_ff2)


def solution(mesh):
    n, tps = mesh.shape["fs"] // 2, mesh.shape["tp"]
    return jax.shard_map(
        functools.partial(local, n, tps),
        mesh=mesh,
        in_specs=(
            P("fs", "tp"),
            P("tp"),
            P("fs", "tp"),
            P("tp"),
            P("fs", "tp"),
            P("tp"),
            P("fs", "tp"),
            P("fs", "tp"),
            P("tp"),
        ),
        out_specs=P("fs", "tp"),
        check_vma=False,
    )
```
